32 devices in a mesh: grp: 2 (over y), sp: 4 (over z), fs: 2 (over x), tp: 2 (over core).
Axes of the slice: x: 2, y: 2, z: 4, core: 2. Of those that a mesh axis runs over, the one named last changes fastest.
Arguments:
- tokens: bfloat16 [2, 6144, 2048], P('fs', ('grp', 'sp'), 'tp'), parts along dimension 1, may hold values from -12 to 12
- norm_gain: float32 [2048], replicated, may hold values from 0.1 to 1.9
- query_weight: bfloat16 [2048, 16, 64], P(None, 'tp'), may hold values from -3 to 3
- key_weight: bfloat16 [2048, 4, 64], P(None, 'tp'), may hold values from -3 to 3
- value_weight: bfloat16 [2048, 4, 64], P(None, 'tp'), may hold values from -0.125 to 0.125
- sink_logit: float32 [16], P('tp'), may hold values from 1 to 6
- pool_weight: bfloat16 [2048, 4, 256], P(None, None, 'tp'), may hold values from -0.125 to 0.125
- attn_out_weight: bfloat16 [16, 64, 2048], P('tp'), may hold values from -0.5 to 0.5
- pool_out_weight: bfloat16 [4, 256, 2048], P(None, 'tp'), may hold values from -0.1875 to 0.1875
Outputs:
- mixed: bfloat16 [2, 6144, 2048], P('fs', ('grp', 'sp', 'tp')), parts along dimension 1
The draws below stay inside these ranges and needn't reach their ends.
There are 2 independent parts, one for each index of `grp`. The reference program is written for one: setup_inputs(seed, part) draws one part's arguments, and reference() takes and returns one part's arrays. A program takes and returns all parts, laid end to end along the dimension named above; an argument that names none is the same for every part. Nothing has to cross between parts.
All inputs are finite; a program needn't handle non-finite values.
Results may differ from the reference program's by a relative error of at most 0.0095.
The reference program's roundings to bfloat16 on the way (of `normed`, `weight`, `attended` and `pooled`) count: a program that leaves them out, or rounds other values in their place, can miss the bound.
Values may be sent and summed in bfloat16 or wider, within the bound.
A program may use at most 128 MiB of HBM per device.

```python
import jax
import jax.numpy as jnp
from jax import lax

D = 2048
HEADS = 16
KV_HEADS = 4
HEAD_DIM = 64
POOL_CH = 256
WINDOW = 128
TOK_DEV = 768
SEQS = 2
LEN = 3072


def draw_tokens(key, part):
    first, second, third = jax.random.split(jax.random.fold_in(key, 11), 3)
    blocks = LEN // TOK_DEV
    base = jax.random.normal(first, (SEQS, blocks, TOK_DEV, D), jnp.float32)
    offset = jax.random.normal(second, (SEQS, 1, 1, D), jnp.float32)
    factor = jax.random.uniform(third, (SEQS, blocks, 1, 1), jnp.float32, -1.5, 1.5)
    values = jnp.clip(base + factor * offset, -12.0, 12.0)
    return values.reshape(SEQS, LEN, D).astype(jnp.bfloat16)


def projection(key, heads):
    values = jax.random.normal(key, (D, heads, HEAD_DIM), jnp.float32) * D ** (-0.5)
    return jnp.clip(values, -3.0, 3.0).astype(jnp.bfloat16)


def draw_query_weight(key, part):
    return projection(jax.random.fold_in(key, 21), HEADS)


def draw_key_weight(key, part):
    return projection(jax.random.fold_in(key, 31), KV_HEADS)


def block_levels(stream_key, extent, shards, low, top_value):
    def one(dim, blocks):
        heights = jax.random.uniform(jax.random.fold_in(jax.random.fold_in(stream_key, 6), dim), (blocks,), jnp.float32, low / len(shards), top_value / len(shards))
        return jnp.repeat(jnp.exp(heights), extent[dim] // blocks).reshape((-1,) + (1,) * (len(extent) - dim - 1))

    level = one(*shards[0])
    for cut in shards[1:]:
        level = level * one(*cut)
    return level


def noise(own_key, extent, deviation, limit, cuts=(), kind=jnp.bfloat16):
    loudness = block_levels(own_key, extent, cuts, -0.22, 0.18) if cuts else 1.0
    values = jax.random.normal(own_key, extent, jnp.float32) * deviation * loudness
    return jnp.minimum(jnp.maximum(values, -limit), limit).astype(kind)


def setup_inputs(seed: int = 0, part: int = 0) -> dict:
    streams_of = jax.random.split(jax.random.key(seed), 10)
    part_splits = jax.random.split(jax.random.fold_in(streams_of[9], part), 10)
    tokens = draw_tokens(jax.random.fold_in(jax.random.fold_in(streams_of[9], part), 71), part)
    norm_gain = jnp.clip(1.0 + 0.18 * jax.random.normal(streams_of[1], (D,), jnp.float32), 0.1, 1.9)
    query_weight = draw_query_weight(jax.random.fold_in(streams_of[9], 71), part)
    key_weight = draw_key_weight(jax.random.fold_in(streams_of[9], 71), part)
    value_weight = noise(streams_of[4], (D, KV_HEADS, HEAD_DIM), D ** -0.5, 0.125, ((1, 2),))
    sink_logit = jnp.clip(1.0 + 5.0 * jax.random.uniform(streams_of[5], (HEADS,), jnp.float32) ** block_levels(streams_of[5], (HEADS,), ((0, 2),), -0.2, 0.2), 1.0, 6.0)
    pool_weight = noise(streams_of[6], (D, 4, POOL_CH), D ** -0.5, 0.125, ((2, 2),))
    attn_out_weight = noise(streams_of[7], (HEADS, HEAD_DIM, D), (HEADS * HEAD_DIM // 8) ** -0.5, 0.5, ((0, 2),))
    pool_out_weight = noise(streams_of[8], (4, POOL_CH, D), (4 * POOL_CH) ** -0.5, 0.1875, ((1, 2),))
    return dict(tokens=tokens, norm_gain=norm_gain, query_weight=query_weight, key_weight=key_weight, value_weight=value_weight, sink_logit=sink_logit, pool_weight=pool_weight, attn_out_weight=attn_out_weight, pool_out_weight=pool_out_weight)


def rms_norm(rows, gain):
    values = rows.astype(jnp.float32)
    scale = lax.rsqrt(lax.optimization_barrier(jnp.mean(values * values, axis=-1, keepdims=True)) + 1e-06)
    return (values * scale * gain).astype(jnp.bfloat16)

def attend(query, key, value, sinks):
    group = HEADS // KV_HEADS
    blocks = LEN // WINDOW
    qb = query.reshape(blocks, WINDOW, KV_HEADS, group, HEAD_DIM).astype(jnp.float32)

    def banded(tensor):
        tb = tensor.reshape(blocks, WINDOW, KV_HEADS, HEAD_DIM)
        before = jnp.concatenate([jnp.zeros_like(tb[:1]), tb[:-1]], axis=0)
        return jnp.concatenate([before, tb], axis=1).astype(jnp.float32)
    kw = banded(key)
    vw = banded(value)
    qi = jnp.arange(WINDOW, dtype=jnp.int32)[:, None]
    kj = jnp.arange(2 * WINDOW, dtype=jnp.int32)[None, :]
    dist = WINDOW + qi - kj
    inside = (dist >= 0) & (dist < WINDOW)
    key_pos = jnp.arange(blocks, dtype=jnp.int32)[:, None, None] * WINDOW - WINDOW + kj[None]
    mask = inside[None] & (key_pos >= 0)
    scores = jnp.einsum('nqhgd,nkhd->nhgqk', qb, kw) * HEAD_DIM ** (-0.5)
    scores = jnp.where(mask[:, None, None], scores, -jnp.inf)
    sink = sinks.reshape(1, KV_HEADS, group, 1, 1)
    top = jnp.maximum(lax.optimization_barrier(jnp.max(scores, axis=-1, keepdims=True)), sink)
    expo = jnp.exp(scores - top)
    total = lax.optimization_barrier(jnp.sum(expo, axis=-1, keepdims=True)) + jnp.exp(sink - top)
    weight = (expo / total).astype(jnp.bfloat16)
    out = jnp.einsum('nhgqk,nkhd->nqhgd', weight.astype(jnp.float32), vw)
    return out.reshape(LEN, HEADS * HEAD_DIM).astype(jnp.bfloat16)

def pool(pooled_in):
    values = pooled_in.astype(jnp.float32)
    sums = jnp.cumsum(values, axis=0)
    count = jnp.arange(1, LEN + 1).astype(jnp.float32)[:, None]
    parts = []
    for group, reach in enumerate((2, 4, 16)):
        col = sums[:, group]
        lower = jnp.concatenate([jnp.zeros((reach, POOL_CH), jnp.float32), col[:-reach]], axis=0)
        parts.append((col - lower) / jnp.minimum(count, float(reach)))
    parts.append(sums[:, 3] / count)
    mean = jnp.stack(parts, axis=1)
    return (mean - values).astype(jnp.bfloat16)

def one_sequence(rows, norm_gain, query_weight, key_weight, value_weight, sink_logit, pool_weight, attn_out_weight, pool_out_weight):
    normed = rms_norm(rows, norm_gain)
    query = jnp.dot(normed, query_weight.reshape(D, -1), preferred_element_type=jnp.float32).astype(jnp.bfloat16)
    key = jnp.dot(normed, key_weight.reshape(D, -1), preferred_element_type=jnp.float32).astype(jnp.bfloat16)
    value = jnp.dot(normed, value_weight.reshape(D, -1), preferred_element_type=jnp.float32).astype(jnp.bfloat16)
    pooled_in = jnp.dot(normed, pool_weight.reshape(D, -1), preferred_element_type=jnp.float32).astype(jnp.bfloat16)
    attended = attend(query, key, value, sink_logit)
    pooled = pool(pooled_in.reshape(LEN, 4, POOL_CH)).reshape(LEN, 4 * POOL_CH)
    total = jnp.dot(attended, attn_out_weight.reshape(-1, D), preferred_element_type=jnp.float32)
    total = total + jnp.dot(pooled, pool_out_weight.reshape(-1, D), preferred_element_type=jnp.float32)
    return total.astype(jnp.bfloat16)

def reference(tokens, norm_gain, query_weight, key_weight, value_weight, sink_logit, pool_weight, attn_out_weight, pool_out_weight):

    def apply(rows):
        return one_sequence(rows, norm_gain, query_weight, key_weight, value_weight, sink_logit, pool_weight, attn_out_weight, pool_out_weight)
    return lax.map(apply, tokens)
```

```python
import functools

import jax
import jax.numpy as jnp
from jax import lax
from jax.experimental import pallas as pl
from jax.experimental.pallas import tpu as pltpu
from jax.sharding import PartitionSpec as P

MESH = pl.DeviceIdType.MESH
WINDOW = 128
REACHES = (2, 4, 16)
TAIL = 16
CHUNK = 256
COLS = 512
F32 = jnp.float32
BF16 = jnp.bfloat16


def dot(a, b, dims=((1,), (0,))):
    return lax.dot_general(a, b, (dims, ((), ())), preferred_element_type=F32)


def kernel(
    n_sp,
    heads,
    local_kv,
    head_dim,
    tokens,
    gain,
    wq,
    wk,
    wv,
    sink,
    wp,
    wo,
    wpo,
    out,
    tok,
    normed,
    wqkv,
    wp_raw,
    wp_f32,
    wpool,
    wout,
    qt,
    kvt,
    ext,
    bands,
    block_sum,
    totals,
    act,
    sending,
    landing,
    result,
    w_sem,
    tok_sem,
    tok_send,
    tok_recv,
    halo_send,
    halo_recv,
    tot_send,
    tot_recv,
    out_send,
    out_recv,
    out_sem,
):
    me_sp = lax.axis_index("sp")
    me_tp = lax.axis_index("tp")
    other = 1 - me_tp
    rows, half_width = tokens.shape
    width = 2 * half_width
    q_rows = heads * head_dim
    kv_rows = local_kv * head_dim
    pool_cols = wpool.shape[1]
    channels = pool_cols // 4
    blocks = rows // WINDOW
    chunks = rows // CHUNK
    per_chunk = CHUNK // WINDOW
    half_rows = rows // 2
    half_blocks = blocks // 2
    tiles = width // COLS
    group = heads // local_kv

    barrier = pltpu.get_barrier_semaphore()
    pl.semaphore_signal(barrier, inc=1, device_id={"tp": other}, device_id_type=MESH)
    for step in range(1, n_sp):
        peer = lax.rem(me_sp + step, n_sp)
        pl.semaphore_signal(barrier, inc=1, device_id={"sp": peer}, device_id_type=MESH)

    load_wp = pltpu.make_async_copy(wp, wp_raw, w_sem.at[0])
    load_wp.start()

    def local_tokens(c):
        at = pl.ds(pl.multiple_of(c * CHUNK, CHUNK), CHUNK)
        return pltpu.make_async_copy(tokens.at[at, :], tok.at[me_tp, at, :], tok_sem.at[c])

    def remote_tokens(c):
        at = pl.ds(pl.multiple_of(c * CHUNK, CHUNK), CHUNK)
        return pltpu.make_async_remote_copy(
            src_ref=tokens.at[at, :],
            dst_ref=tok.at[me_tp, at, :],
            send_sem=tok_send.at[c],
            recv_sem=tok_recv.at[c],
            device_id={"tp": other},
            device_id_type=MESH,
        )

    for c in reversed(range(chunks)):
        local_tokens(c).start()
    loads = [
        pltpu.make_async_copy(wq, wqkv.at[pl.ds(0, q_rows), :], w_sem.at[1]),
        pltpu.make_async_copy(wk, wqkv.at[pl.ds(q_rows, kv_rows), :], w_sem.at[2]),
        pltpu.make_async_copy(wv, wqkv.at[pl.ds(q_rows + kv_rows, kv_rows), :], w_sem.at[3]),
    ]
    load_out = [
        pltpu.make_async_copy(wo, wout.at[pl.ds(0, q_rows), :], w_sem.at[4]),
        pltpu.make_async_copy(wpo, wout.at[pl.ds(q_rows, pool_cols), :], w_sem.at[5]),
    ]
    for load in loads:
        load.start()

    target = lax.broadcasted_iota(jnp.int32, (WINDOW, 2 * WINDOW), 0) + WINDOW
    source = lax.broadcasted_iota(jnp.int32, (WINDOW, 2 * WINDOW), 1)
    gap = target - source
    for g, reach in enumerate(REACHES):
        bands[g] = jnp.where((gap >= 0) & (gap < reach), 1.0, 0.0).astype(BF16)
    bands[3] = jnp.where((gap >= 0) & (gap < WINDOW) & (source >= WINDOW), 1.0, 0.0).astype(BF16)
    ext[pl.ds(0, WINDOW - TAIL), :] = jnp.zeros((WINDOW - TAIL, pool_cols), BF16)

    @pl.when(me_sp == 0)
    def _():
        ext[pl.ds(WINDOW - TAIL, TAIL), :] = jnp.zeros((TAIL, pool_cols), BF16)
        kvt[0] = jnp.zeros((2 * kv_rows, WINDOW), BF16)

    pl.semaphore_wait(barrier, n_sp)
    for c in reversed(range(chunks)):
        remote_tokens(c).start()
    for load in load_out:
        load.start()

    load_wp.wait()
    part = wp_f32.shape[0]

    def regroup(i, carry):
        wp_f32[...] = wp_raw[pl.ds(pl.multiple_of(i * part, part), part), :].astype(F32)
        at = pl.ds(pl.multiple_of(i * (part // 4), part // 4), part // 4)
        for g in range(4):
            wpool[at, pl.ds(g * channels, channels)] = wp_f32[
                pl.ds(g, part // 4, stride=4), :
            ].astype(BF16)
        return carry

    lax.fori_loop(0, wp_raw.shape[0] // part, regroup, 0)
    for load in loads:
        load.wait()

    halo_kv = pltpu.make_async_remote_copy(
        src_ref=kvt.at[blocks],
        dst_ref=kvt.at[0],
        send_sem=halo_send.at[0],
        recv_sem=halo_recv.at[0],
        device_id={"sp": lax.rem(me_sp + 1, n_sp)},
        device_id_type=MESH,
    )
    halo_pool = pltpu.make_async_remote_copy(
        src_ref=ext.at[pl.ds(WINDOW + rows - TAIL, TAIL), :],
        dst_ref=ext.at[pl.ds(WINDOW - TAIL, TAIL), :],
        send_sem=halo_send.at[1],
        recv_sem=halo_recv.at[1],
        device_id={"sp": lax.rem(me_sp + 1, n_sp)},
        device_id_type=MESH,
    )

    scale = head_dim ** (-0.5)

    def project(i, carry):
        c = chunks - 1 - i
        local_tokens(c).wait()
        remote_tokens(c).wait_recv()
        at = pl.ds(pl.multiple_of(c * CHUNK, CHUNK), CHUNK)
        low = tok[0, at, :].astype(F32)
        high = tok[1, at, :].astype(F32)
        square = jnp.sum(low * low, axis=1, keepdims=True)
        square = square + jnp.sum(high * high, axis=1, keepdims=True)
        inv = lax.rsqrt(square * (1.0 / width) + 1e-06)
        normed[:, pl.ds(0, half_width)] = (low * inv * gain[:, pl.ds(0, half_width)]).astype(BF16)
        normed[:, pl.ds(half_width, half_width)] = (
            high * inv * gain[:, pl.ds(half_width, half_width)]
        ).astype(BF16)

        @pl.when((i == 1) & (me_sp < n_sp - 1))
        def _():
            halo_kv.start()
            halo_pool.start()

        pooled_in = dot(normed[...], wpool[...]).astype(BF16)
        ext[pl.ds(pl.multiple_of(WINDOW + c * CHUNK, WINDOW), CHUNK), :] = pooled_in
        last = pooled_in[:, 3 * channels :].astype(F32)
        for j in range(per_chunk):
            summed = jnp.sum(last[j * WINDOW : (j + 1) * WINDOW], axis=0, keepdims=True)
            block_sum[c * per_chunk + j] = jnp.broadcast_to(summed, (8, channels))
        qkv = dot(wqkv[...], normed[...], ((1,), (1,)))
        for j in range(per_chunk):
            b = c * per_chunk + j
            piece = qkv[:, j * WINDOW : (j + 1) * WINDOW]
            qt[b] = (piece[:q_rows] * scale).astype(BF16)
            kvt[b + 1] = piece[q_rows:].astype(BF16)
        return carry

    lax.fori_loop(0, chunks, project, 0)

    all_rows = block_sum[0]
    for b in range(1, blocks):
        all_rows = all_rows + block_sum[b]
    totals[me_sp] = all_rows
    sends = []
    for step in range(1, n_sp):
        peer = lax.rem(me_sp + step, n_sp)
        sends.append(
            pltpu.make_async_remote_copy(
                src_ref=totals.at[me_sp],
                dst_ref=totals.at[me_sp],
                send_sem=tot_send.at[step],
                recv_sem=tot_recv.at[step],
                device_id={"sp": peer},
                device_id_type=MESH,
            )
        )

    key_at = lax.broadcasted_iota(jnp.int32, (WINDOW, group * WINDOW), 0)
    query_at = lax.rem(
        lax.broadcasted_iota(jnp.int32, (WINDOW, group * WINDOW), 1), jnp.int32(WINDOW)
    )
    own_key = key_at <= query_at

    def attend(b, slot):
        bias = jnp.where((b == 0) & (me_sp == 0), -jnp.inf, 0.0).astype(F32)
        parts = []
        for h in range(local_kv):
            q = jnp.concatenate(
                [
                    qt[b, pl.ds((h * group + g) * head_dim, head_dim), :]
                    for g in range(group)
                ],
                axis=1,
            )
            s = jnp.concatenate(
                [jnp.full((1, WINDOW), sink[h * group + g], F32) for g in range(group)], axis=1
            )
            k_at = pl.ds(h * head_dim, head_dim)
            v_at = pl.ds(kv_rows + h * head_dim, head_dim)
            before = dot(kvt[b, k_at, :], q, ((0,), (0,))) + bias
            own = dot(kvt[b + 1, k_at, :], q, ((0,), (0,)))
            score = jnp.where(own_key, own, before)
            top = jnp.maximum(jnp.max(score, axis=0, keepdims=True), s)
            expo = jnp.exp(score - top)
            total = jnp.sum(expo, axis=0, keepdims=True) + jnp.exp(s - top)
            weight = expo * (1.0 / total)
            w_before = jnp.where(own_key, 0.0, weight).astype(BF16)
            w_own = jnp.where(own_key, weight, 0.0).astype(BF16)
            gathered = dot(kvt[b, v_at, :], w_before) + dot(kvt[b + 1, v_at, :], w_own)
            parts += [gathered[:, g * WINDOW : (g + 1) * WINDOW] for g in range(group)]
        attended = jnp.concatenate(parts, axis=0)
        act[pl.ds(pl.multiple_of(slot * WINDOW, WINDOW), WINDOW), pl.ds(0, q_rows)] = (
            attended.T.astype(BF16)
        )

    def pool(b, slot, carried):
        start = pl.multiple_of(b * WINDOW, WINDOW)
        position = me_sp * rows + b * WINDOW + 1
        count = (lax.broadcasted_iota(jnp.int32, (WINDOW, channels), 0) + position).astype(F32)
        at = pl.ds(pl.multiple_of(slot * WINDOW, WINDOW), WINDOW)
        for g in range(4):
            col = pl.ds(g * channels, channels)
            own = ext[pl.ds(start + WINDOW, WINDOW), col]
            if g < 3:
                sums = dot(bands[g], ext[pl.ds(start, 2 * WINDOW), col])
                denom = jnp.minimum(count, float(REACHES[g]))
            else:
                base = carried
                for earlier in range(blocks):
                    base = base + jnp.where(earlier < b, block_sum[earlier], 0.0)
                sums = dot(bands[3, :, pl.ds(WINDOW, WINDOW)], own) + base[:1]
                denom = count
            pooled = sums * (1.0 / denom) - own.astype(F32)
            act[at, pl.ds(q_rows + g * channels, channels)] = pooled.astype(BF16)

    for send in sends:
        send.start()

    @pl.when(me_sp > 0)
    def _():
        halo_kv.wait_recv()
        halo_pool.wait_recv()

    def attend_half(first):
        def one(i, carry):
            attend(first + i, i)
            return carry

        lax.fori_loop(0, half_blocks, one, 0)

    def pool_half(first, carried):
        def one(i, carry):
            pool(first + i, i, carried)
            return carry

        lax.fori_loop(0, half_blocks, one, 0)

    first = other * half_blocks
    attend_half(first)
    for send in sends:
        send.wait()
    carried = jnp.zeros((8, channels), F32)
    for index in range(n_sp):
        carried = carried + jnp.where(index < me_sp, totals[index], 0.0)
    pool_half(first, carried)
    for load in load_out:
        load.wait()

    def partial_send(t):
        return pltpu.make_async_remote_copy(
            src_ref=sending.at[t],
            dst_ref=landing.at[t],
            send_sem=out_send.at[t],
            recv_sem=out_recv.at[t],
            device_id={"tp": other},
            device_id_type=MESH,
        )

    def columns(t):
        return pl.ds(pl.multiple_of(t * COLS, COLS), COLS)

    def give(t, carry):
        sending[t] = dot(act[...], wout[:, columns(t)]).astype(BF16)
        partial_send(t).start()
        return carry

    lax.fori_loop(0, tiles, give, 0)

    first = me_tp * half_blocks
    attend_half(first)
    pool_half(first, carried)

    def store(t):
        return pltpu.make_async_copy(result.at[t], out.at[:, columns(t)], out_sem.at[t])

    def keep(t, carry):
        partial_send(t).wait_recv()
        mine = dot(act[...], wout[:, columns(t)])
        result[t] = (mine + landing[t].astype(F32)).astype(BF16)
        store(t).start()
        return carry

    lax.fori_loop(0, tiles, keep, 0)
    for t in range(tiles):
        store(t).wait()
        partial_send(t).wait_send()
    for c in range(chunks):
        remote_tokens(c).wait_send()

    @pl.when(me_sp < n_sp - 1)
    def _():
        halo_kv.wait_send()
        halo_pool.wait_send()


def shards(n_sp, tokens, gain, wq, wk, wv, sink, wp, wo, wpo):
    rows, half_width = tokens.shape[1:]
    width = 2 * half_width
    heads, head_dim = wq.shape[1:]
    local_kv = wk.shape[1]
    channels = wp.shape[2]
    q_rows, kv_rows = (heads * head_dim, local_kv * head_dim)
    pool_cols = 4 * channels
    blocks = rows // WINDOW
    tiles = width // COLS
    chunks = rows // CHUNK
    dma = pltpu.SemaphoreType.DMA
    flat = lambda w: jnp.transpose(w, (1, 2, 0)).reshape(-1, width)
    hbm = pl.BlockSpec(memory_space=pl.ANY)
    vmem = pl.BlockSpec(memory_space=pltpu.VMEM)
    smem = pl.BlockSpec(memory_space=pltpu.SMEM)
    result = pl.pallas_call(
        functools.partial(kernel, n_sp, heads, local_kv, head_dim),
        out_shape=jax.ShapeDtypeStruct((rows // 2, width), BF16),
        in_specs=[hbm, vmem, hbm, hbm, hbm, smem, hbm, hbm, hbm],
        out_specs=hbm,
        scratch_shapes=[
            pltpu.VMEM((2, rows, half_width), BF16),
            pltpu.VMEM((CHUNK, width), BF16),
            pltpu.VMEM((q_rows + 2 * kv_rows, width), BF16),
            pltpu.VMEM((4 * width, channels), BF16),
            pltpu.VMEM((1024, channels), F32),
            pltpu.VMEM((width, pool_cols), BF16),
            pltpu.VMEM((q_rows + pool_cols, width), BF16),
            pltpu.VMEM((blocks, q_rows, WINDOW), BF16),
            pltpu.VMEM((blocks + 1, 2 * kv_rows, WINDOW), BF16),
            pltpu.VMEM((rows + WINDOW, pool_cols), BF16),
            pltpu.VMEM((4, WINDOW, 2 * WINDOW), BF16),
            pltpu.VMEM((blocks, 8, channels), F32),
            pltpu.VMEM((n_sp, 8, channels), F32),
            pltpu.VMEM((rows // 2, q_rows + pool_cols), BF16),
            pltpu.VMEM((tiles, rows // 2, COLS), BF16),
            pltpu.VMEM((tiles, rows // 2, COLS), BF16),
            pltpu.VMEM((tiles, rows // 2, COLS), BF16),
            dma((6,)),
            dma((chunks,)),
            dma((chunks,)),
            dma((chunks,)),
            dma((2,)),
            dma((2,)),
            dma((n_sp,)),
            dma((n_sp,)),
            dma((tiles,)),
            dma((tiles,)),
            dma((tiles,)),
        ],
        compiler_params=pltpu.CompilerParams(
            collective_id=0, has_side_effects=True, vmem_limit_bytes=60 * 1024 * 1024
        ),
    )(
        tokens[0],
        gain.reshape(1, width),
        flat(wq),
        flat(wk),
        flat(wv),
        sink,
        wp.reshape(-1, channels),
        wo.reshape(-1, width),
        wpo.reshape(-1, width),
    )
    return result[None]


def solution(mesh):
    in_specs = (
        P("fs", ("grp", "sp"), "tp"),
        P(),
        P(None, "tp", None),
        P(None, "tp", None),
        P(None, "tp", None),
        P("tp"),
        P(None, None, "tp"),
        P("tp", None, None),
        P(None, "tp", None),
    )
    out_specs = P("fs", ("grp", "sp", "tp"), None)
    return jax.shard_map(
        functools.partial(shards, mesh.shape["sp"]),
        mesh=mesh,
        in_specs=in_specs,
        out_specs=out_specs,
        check_vma=False,
    )
```

```python
import functools

import jax
import jax.numpy as jnp
from jax import lax
from jax.experimental import pallas as pl
from jax.experimental.pallas import tpu as pltpu
from jax.sharding import PartitionSpec as P

MESH = pl.DeviceIdType.MESH
WINDOW = 128
REACHES = (2, 4, 16)
TAIL = 16
CHUNK = 256
COLS = 512
F32 = jnp.float32
BF16 = jnp.bfloat16


def dot(a, b, dims=((1,), (0,))):
    return lax.dot_general(a, b, (dims, ((), ())), preferred_element_type=F32)


def kernel(
    n_sp,
    heads,
    local_kv,
    head_dim,
    tokens,
    gain,
    wq,
    wk,
    wv,
    sink,
    wp,
    wo,
    wpo,
    out,
    tok,
    normed,
    wqkv,
    wp_raw,
    wp_f32,
    wpool,
    wout,
    qt,
    kvt,
    ext,
    bands,
    block_sum,
    totals,
    act,
    sending,
    landing,
    w_sem,
    tok_sem,
    tok_send,
    tok_recv,
    halo_send,
    halo_recv,
    tot_send,
    tot_recv,
    out_send,
    out_recv,
    entered,
):
    me_sp = lax.axis_index("sp")
    me_tp = lax.axis_index("tp")
    other = 1 - me_tp
    rows, half_width = tokens.shape
    width = 2 * half_width
    q_rows = heads * head_dim
    kv_rows = local_kv * head_dim
    pool_cols = wpool.shape[1]
    channels = pool_cols // 4
    blocks = rows // WINDOW
    chunks = rows // CHUNK
    per_chunk = CHUNK // WINDOW
    half_rows = rows // 2
    half_blocks = blocks // 2
    tiles = width // COLS
    group = heads // local_kv

    for index in range(n_sp):
        totals[index] = jnp.zeros((8, channels), F32)
    barrier = pltpu.get_barrier_semaphore()
    pl.semaphore_signal(barrier, inc=1, device_id={"tp": other}, device_id_type=MESH)

    @pl.when(me_sp > 0)
    def _():
        pl.semaphore_signal(barrier, inc=1, device_id={"sp": me_sp - 1}, device_id_type=MESH)

    @pl.when(me_sp < n_sp - 1)
    def _():
        pl.semaphore_signal(barrier, inc=1, device_id={"sp": me_sp + 1}, device_id_type=MESH)

    load_wp = pltpu.make_async_copy(wp, wp_raw, w_sem.at[0])

    def local_tokens(c):
        at = pl.ds(pl.multiple_of(c * CHUNK, CHUNK), CHUNK)
        return pltpu.make_async_copy(tokens.at[at, :], tok.at[me_tp, at, :], tok_sem.at[c])

    def remote_tokens(c):
        at = pl.ds(pl.multiple_of(c * CHUNK, CHUNK), CHUNK)
        return pltpu.make_async_remote_copy(
            src_ref=tokens.at[at, :],
            dst_ref=tok.at[me_tp, at, :],
            send_sem=tok_send.at[c],
            recv_sem=tok_recv.at[c],
            device_id={"tp": other},
            device_id_type=MESH,
        )

    for c in reversed(range(chunks)):
        local_tokens(c).start()
    load_wp.start()
    loads = [
        pltpu.make_async_copy(wq, wqkv.at[pl.ds(0, q_rows), :], w_sem.at[1]),
        pltpu.make_async_copy(wk, wqkv.at[pl.ds(q_rows, kv_rows), :], w_sem.at[2]),
        pltpu.make_async_copy(wv, wqkv.at[pl.ds(q_rows + kv_rows, kv_rows), :], w_sem.at[3]),
    ]
    load_out = [
        pltpu.make_async_copy(wo, wout.at[pl.ds(0, q_rows), :], w_sem.at[4]),
        pltpu.make_async_copy(wpo, wout.at[pl.ds(q_rows, pool_cols), :], w_sem.at[5]),
    ]
    for load in loads:
        load.start()

    target = lax.broadcasted_iota(jnp.int32, (WINDOW, 2 * WINDOW), 0) + WINDOW
    source = lax.broadcasted_iota(jnp.int32, (WINDOW, 2 * WINDOW), 1)
    gap = target - source
    for g, reach in enumerate(REACHES):
        bands[g] = jnp.where((gap >= 0) & (gap < reach), 1.0, 0.0).astype(BF16)
    bands[3] = jnp.where((gap >= 0) & (gap < WINDOW) & (source >= WINDOW), 1.0, 0.0).astype(BF16)
    ext[pl.ds(0, WINDOW - TAIL), :] = jnp.zeros((WINDOW - TAIL, pool_cols), BF16)

    @pl.when(me_sp == 0)
    def _():
        ext[pl.ds(WINDOW - TAIL, TAIL), :] = jnp.zeros((TAIL, pool_cols), BF16)
        kvt[0] = jnp.zeros((2 * kv_rows, WINDOW), BF16)

    neighbours = jnp.where(me_sp > 0, 1, 0) + jnp.where(me_sp < n_sp - 1, 1, 0)
    pl.semaphore_wait(barrier, 1 + neighbours)
    for c in reversed(range(chunks)):
        remote_tokens(c).start()
    for load in load_out:
        load.start()

    load_wp.wait()
    part = wp_f32.shape[0]

    def regroup(i, carry):
        wp_f32[...] = wp_raw[pl.ds(pl.multiple_of(i * part, part), part), :].astype(F32)
        at = pl.ds(pl.multiple_of(i * (part // 4), part // 4), part // 4)
        for g in range(4):
            wpool[at, pl.ds(g * channels, channels)] = wp_f32[
                pl.ds(g, part // 4, stride=4), :
            ].astype(BF16)
        return carry

    lax.fori_loop(0, wp_raw.shape[0] // part, regroup, 0)
    for load in loads:
        load.wait()

    halo_kv = pltpu.make_async_remote_copy(
        src_ref=kvt.at[blocks],
        dst_ref=kvt.at[0],
        send_sem=halo_send.at[0],
        recv_sem=halo_recv.at[0],
        device_id={"sp": lax.rem(me_sp + 1, n_sp)},
        device_id_type=MESH,
    )
    halo_pool = pltpu.make_async_remote_copy(
        src_ref=ext.at[pl.ds(WINDOW + rows - TAIL, TAIL), :],
        dst_ref=ext.at[pl.ds(WINDOW - TAIL, TAIL), :],
        send_sem=halo_send.at[1],
        recv_sem=halo_recv.at[1],
        device_id={"sp": lax.rem(me_sp + 1, n_sp)},
        device_id_type=MESH,
    )

    scale = head_dim ** (-0.5)

    def normalize(c):
        local_tokens(c).wait()
        remote_tokens(c).wait_recv()
        at = pl.ds(pl.multiple_of(c * CHUNK, CHUNK), CHUNK)
        low = tok[0, at, :].astype(F32)
        high = tok[1, at, :].astype(F32)
        square = jnp.sum(low * low, axis=1, keepdims=True)
        square = square + jnp.sum(high * high, axis=1, keepdims=True)
        inv = lax.rsqrt(square * (1.0 / width) + 1e-06)
        normed[c, :, pl.ds(0, half_width)] = (low * inv * gain[:, pl.ds(0, half_width)]).astype(
            BF16
        )
        normed[c, :, pl.ds(half_width, half_width)] = (
            high * inv * gain[:, pl.ds(half_width, half_width)]
        ).astype(BF16)

    def project_pool(c):
        pooled_in = dot(normed[c], wpool[...]).astype(BF16)
        ext[pl.ds(pl.multiple_of(WINDOW + c * CHUNK, WINDOW), CHUNK), :] = pooled_in
        last = pooled_in[:, 3 * channels :].astype(F32)
        for j in range(per_chunk):
            summed = jnp.sum(last[j * WINDOW : (j + 1) * WINDOW], axis=0, keepdims=True)
            block_sum[c * per_chunk + j] = jnp.broadcast_to(summed, (8, channels))

    def project_qkv(c):
        qkv = dot(wqkv[...], normed[c], ((1,), (1,)))
        for j in range(per_chunk):
            b = c * per_chunk + j
            piece = qkv[:, j * WINDOW : (j + 1) * WINDOW]
            qt[b] = (piece[:q_rows] * scale).astype(BF16)
            kvt[b + 1] = piece[q_rows:].astype(BF16)

    def hear(step):
        @pl.when(me_sp + step < n_sp - 1)
        def _():
            pl.semaphore_wait(entered.at[step], 1)

    def tell(step):
        @pl.when((me_sp > 0) & (me_sp + step - 1 < n_sp - 1))
        def _():
            pl.semaphore_signal(
                entered.at[step], inc=1, device_id={"sp": me_sp - 1}, device_id_type=MESH
            )

    if n_sp > 2:
        tell(1)

    def project(i, carry):
        c = chunks - 1 - i
        normalize(c)

        @pl.when((i == 1) & (me_sp < n_sp - 1))
        def _():
            halo_kv.start()
            halo_pool.start()

        @pl.when(i > 0)
        def _():
            hear(i)
            tell(i + 1)

        project_pool(c)
        project_qkv(c)
        return carry

    lax.fori_loop(0, chunks, project, 0)

    for step in range(chunks, n_sp - 1):
        hear(step)
        if step < n_sp - 2:
            tell(step + 1)

    all_rows = block_sum[0]
    for b in range(1, blocks):
        all_rows = all_rows + block_sum[b]
    totals[me_sp] = all_rows

    def total_copy(step):
        return pltpu.make_async_remote_copy(
            src_ref=totals.at[me_sp],
            dst_ref=totals.at[me_sp],
            send_sem=tot_send.at[step],
            recv_sem=tot_recv.at[step],
            device_id={"sp": lax.rem(me_sp + step, n_sp)},
            device_id_type=MESH,
        )

    for step in range(1, n_sp):

        @pl.when(me_sp + step < n_sp)
        def _():
            total_copy(step).start()

    key_at = lax.broadcasted_iota(jnp.int32, (WINDOW, group * WINDOW), 0)
    query_at = lax.rem(
        lax.broadcasted_iota(jnp.int32, (WINDOW, group * WINDOW), 1), jnp.int32(WINDOW)
    )
    own_key = key_at <= query_at

    def attend(b, slot):
        bias = jnp.where((b == 0) & (me_sp == 0), -jnp.inf, 0.0).astype(F32)
        parts = []
        for h in range(local_kv):
            q = jnp.concatenate(
                [
                    qt[b, pl.ds((h * group + g) * head_dim, head_dim), :]
                    for g in range(group)
                ],
                axis=1,
            )
            s = jnp.concatenate(
                [jnp.full((1, WINDOW), sink[h * group + g], F32) for g in range(group)], axis=1
            )
            k_at = pl.ds(h * head_dim, head_dim)
            v_at = pl.ds(kv_rows + h * head_dim, head_dim)
            before = dot(kvt[b, k_at, :], q, ((0,), (0,))) + bias
            own = dot(kvt[b + 1, k_at, :], q, ((0,), (0,)))
            score = jnp.where(own_key, own, before)
            top = jnp.maximum(jnp.max(score, axis=0, keepdims=True), s)
            expo = jnp.exp(score - top)
            total = jnp.sum(expo, axis=0, keepdims=True) + jnp.exp(s - top)
            weight = expo * (1.0 / total)
            w_before = jnp.where(own_key, 0.0, weight).astype(BF16)
            w_own = jnp.where(own_key, weight, 0.0).astype(BF16)
            gathered = dot(kvt[b, v_at, :], w_before) + dot(kvt[b + 1, v_at, :], w_own)
            parts += [gathered[:, g * WINDOW : (g + 1) * WINDOW] for g in range(group)]
        attended = jnp.concatenate(parts, axis=0)
        act[pl.ds(pl.multiple_of(slot * WINDOW, WINDOW), WINDOW), pl.ds(0, q_rows)] = (
            attended.T.astype(BF16)
        )

    def pool(b, slot, carried):
        start = pl.multiple_of(b * WINDOW, WINDOW)
        position = me_sp * rows + b * WINDOW + 1
        count = (lax.broadcasted_iota(jnp.int32, (WINDOW, channels), 0) + position).astype(F32)
        at = pl.ds(pl.multiple_of(slot * WINDOW, WINDOW), WINDOW)
        for g in range(4):
            col = pl.ds(g * channels, channels)
            own = ext[pl.ds(start + WINDOW, WINDOW), col]
            if g < 3:
                sums = dot(bands[g], ext[pl.ds(start, 2 * WINDOW), col])
                denom = jnp.minimum(count, float(REACHES[g]))
            else:
                base = carried
                for earlier in range(blocks):
                    base = base + jnp.where(earlier < b, block_sum[earlier], 0.0)
                sums = dot(bands[3, :, pl.ds(WINDOW, WINDOW)], own) + base[:1]
                denom = count
            pooled = sums * (1.0 / denom) - own.astype(F32)
            act[at, pl.ds(q_rows + g * channels, channels)] = pooled.astype(BF16)

    @pl.when(me_sp > 0)
    def _():
        halo_kv.wait_recv()
        halo_pool.wait_recv()

    def attend_half(first):
        def one(i, carry):
            attend(first + i, i)
            return carry

        lax.fori_loop(0, half_blocks, one, 0, unroll=True)

    def pool_half(first, carried):
        def one(i, carry):
            pool(first + i, i, carried)
            return carry

        lax.fori_loop(0, half_blocks, one, 0, unroll=True)

    first = other * half_blocks
    attend_half(first)
    for step in range(1, n_sp):

        @pl.when(me_sp - step >= 0)
        def _():
            total_copy(step).wait_recv()

    carried = jnp.zeros((8, channels), F32)
    for index in range(n_sp):
        carried = carried + jnp.where(index < me_sp, totals[index], 0.0)
    pool_half(first, carried)
    for load in load_out:
        load.wait()

    def partial_send(t):
        return pltpu.make_async_remote_copy(
            src_ref=sending.at[t],
            dst_ref=landing.at[t],
            send_sem=out_send.at[t],
            recv_sem=out_recv.at[t],
            device_id={"tp": other},
            device_id_type=MESH,
        )

    def columns(t):
        return pl.ds(pl.multiple_of(t * COLS, COLS), COLS)

    def give(t, carry):
        sending[t] = dot(act[...], wout[:, columns(t)]).astype(BF16)
        partial_send(t).start()
        return carry

    lax.fori_loop(0, tiles, give, 0)

    first = me_tp * half_blocks
    attend_half(first)
    pool_half(first, carried)

    def keep(t, carry):
        partial_send(t).wait_recv()
        mine = dot(act[...], wout[:, columns(t)])
        out[:, columns(t)] = (mine + landing[t].astype(F32)).astype(BF16)
        return carry

    lax.fori_loop(0, tiles, keep, 0)
    for t in range(tiles):
        partial_send(t).wait_send()
    for c in range(chunks):
        remote_tokens(c).wait_send()
    for step in range(1, n_sp):

        @pl.when(me_sp + step < n_sp)
        def _():
            total_copy(step).wait_send()


    @pl.when(me_sp < n_sp - 1)
    def _():
        halo_kv.wait_send()
        halo_pool.wait_send()


def shards(n_sp, tokens, gain, wq, wk, wv, sink, wp, wo, wpo):
    rows, half_width = tokens.shape[1:]
    width = 2 * half_width
    heads, head_dim = wq.shape[1:]
    local_kv = wk.shape[1]
    channels = wp.shape[2]
    q_rows, kv_rows = (heads * head_dim, local_kv * head_dim)
    pool_cols = 4 * channels
    blocks = rows // WINDOW
    tiles = width // COLS
    chunks = rows // CHUNK
    dma = pltpu.SemaphoreType.DMA
    flat = lambda w: jnp.transpose(w, (1, 2, 0)).reshape(-1, width)
    hbm = pl.BlockSpec(memory_space=pltpu.HBM)
    vmem = pl.BlockSpec(memory_space=pltpu.VMEM)
    smem = pl.BlockSpec(memory_space=pltpu.SMEM)
    result = pl.pallas_call(
        functools.partial(kernel, n_sp, heads, local_kv, head_dim),
        out_shape=pltpu.VMEM((rows // 2, width), BF16),
        in_specs=[hbm, vmem, hbm, hbm, hbm, smem, hbm, hbm, hbm],
        out_specs=vmem,
        scratch_shapes=[
            pltpu.VMEM((2, rows, half_width), BF16),
            pltpu.VMEM((chunks, CHUNK, width), BF16),
            pltpu.VMEM((q_rows + 2 * kv_rows, width), BF16),
            pltpu.VMEM((4 * width, channels), BF16),
            pltpu.VMEM((1024, channels), F32),
            pltpu.VMEM((width, pool_cols), BF16),
            pltpu.VMEM((q_rows + pool_cols, width), BF16),
            pltpu.VMEM((blocks, q_rows, WINDOW), BF16),
            pltpu.VMEM((blocks + 1, 2 * kv_rows, WINDOW), BF16),
            pltpu.VMEM((rows + WINDOW, pool_cols), BF16),
            pltpu.VMEM((4, WINDOW, 2 * WINDOW), BF16),
            pltpu.VMEM((blocks, 8, channels), F32),
            pltpu.VMEM((n_sp, 8, channels), F32),
            pltpu.VMEM((rows // 2, q_rows + pool_cols), BF16),
            pltpu.VMEM((tiles, rows // 2, COLS), BF16),
            pltpu.VMEM((tiles, rows // 2, COLS), BF16),
            dma((6,)),
            dma((chunks,)),
            dma((chunks,)),
            dma((chunks,)),
            dma((2,)),
            dma((2,)),
            dma((n_sp,)),
            dma((n_sp,)),
            dma((tiles,)),
            dma((tiles,)),
            pltpu.SemaphoreType.REGULAR((n_sp,)),
        ],
        compiler_params=pltpu.CompilerParams(
            collective_id=0, has_side_effects=True, vmem_limit_bytes=67043328 - rows * width - 65536
        ),
    )(
        tokens[0],
        gain.reshape(1, width),
        flat(wq),
        flat(wk),
        flat(wv),
        sink,
        wp.reshape(-1, channels),
        wo.reshape(-1, width),
        wpo.reshape(-1, width),
    )
    return result[None]


def solution(mesh):
    in_specs = (
        P("fs", ("grp", "sp"), "tp"),
        P(),
        P(None, "tp", None),
        P(None, "tp", None),
        P(None, "tp", None),
        P("tp"),
        P(None, None, "tp"),
        P("tp", None, None),
        P(None, "tp", None),
    )
    out_specs = P("fs", ("grp", "sp", "tp"), None)
    return jax.shard_map(
        functools.partial(shards, mesh.shape["sp"]),
        mesh=mesh,
        in_specs=in_specs,
        out_specs=out_specs,
        check_vma=False,
    )
```
